32 devices in a mesh: sp: 8 (over z, y), tp: 4 (over x, core).
Axes of the slice: x: 2, y: 2, z: 4, core: 2. Of those that a mesh axis runs over, the one named last changes fastest.
Arguments:
- tokens: bfloat16 [2, 4096, 2048], P(None, ('sp', 'tp')), may hold values from -6.5 to 6.5, as said below
- norm_gain: float32 [2048], replicated, may hold values from 0.1 to 1.9
- w_gate: bfloat16 [2048, 4096], P('sp', 'tp'), may hold values from -0.125 to 0.125
- w_value: bfloat16 [2048, 4096], P('sp', 'tp'), may hold values from -0.125 to 0.125
- w_write: bfloat16 [2048, 512], P('sp', 'tp'), may hold values from -0.125 to 0.125
- w_read: bfloat16 [2048, 512], P('sp', 'tp'), may hold values from -0.125 to 0.125
- w_step: bfloat16 [2048, 64], replicated, may hold values from -0.125 to 0.125
- conv_value: float32 [4, 4096], replicated, may hold values from -3 to 3
- conv_write: float32 [4, 512], replicated, may hold values from -3 to 3
- conv_read: float32 [4, 512], replicated, may hold values from -3 to 3
- step_bias: float32 [64], replicated, as said below
- decay_log: float32 [64], replicated, may hold values from 0 to 0.7
- skip_gain: float32 [64], replicated, may hold values from 0.1 to 1.9
- out_gain: float32 [4096], replicated, may hold values from 0.1 to 1.9
- w_out: bfloat16 [4096, 2048], P(None, 'sp'), may hold values from -0.09375 to 0.09375
Outputs:
- mixed: bfloat16 [2, 4096, 2048], P(None, ('sp', 'tp'))
The draws below stay inside these ranges and needn't reach their ends.
Inputs may be any that keep to these rules, and one draw needn't show every extreme that they name: `tokens`: activations of order one whose mean along a direction drifts slowly over each sequence. `step_bias`: even heads take step offsets between -5.8 and -5.0, odd heads offsets near log(0.12 to 0.33) - log(4096).
All inputs are finite; a program needn't handle non-finite values.
Results may differ from the reference program's by a relative error of at most 0.005.
The reference program's roundings to bfloat16 on the way (of `normed`, `gated` and `mixed_in`) count: a program that leaves them out, or rounds other values in their place, can miss the bound.
Values may be sent and summed in bfloat16 or wider, within the bound.
A program may use at most 192 MiB of HBM per device.

```python
import math
import jax
import jax.numpy as jnp
from jax import lax

D = 2048
HEADS = 64
HEAD_DIM = 64
GROUPS = 4
STATE = 128
CONV = 4
BLOCK = 64
SEQS = 2
HW = 4096
LENGTH = 4096


def draw_tokens(key, part):
    key_base, key_dir, key_phase, key_scale = jax.random.split(key, 4)
    base = jax.random.truncated_normal(key_base, -5.0, 5.0, (SEQS, LENGTH, D), jnp.float32)
    direction = jax.random.uniform(key_dir, (D,), jnp.float32, -1.0, 1.0)
    phase = jax.random.uniform(key_phase, (SEQS, 1), jnp.float32, 0.0, 6.283)
    position = jnp.arange(LENGTH, dtype=jnp.float32)[None, :] / LENGTH
    level = 1.5 * jnp.sin(18.85 * position + phase)
    return (base + level[..., None] * direction).astype(jnp.bfloat16)


def draw_step_bias(key, part):
    key_short, key_long = jax.random.split(key)
    short_mem = jax.random.uniform(key_short, (HEADS,), jnp.float32, -5.8, -5.0)
    long_mem = jax.random.uniform(key_long, (HEADS,), jnp.float32, math.log(0.12), math.log(0.33)) - math.log(LENGTH)
    parity = jnp.arange(HEADS) % 2
    return jnp.where(parity == 0, short_mem, long_mem)


def block_levels(stream_key, extent, cuts, low, top_value):
    level, own = 1.0, jax.random.fold_in(stream_key, 6)
    for axis_at, shards_of in cuts:
        heights = jnp.exp(jax.random.uniform(jax.random.fold_in(own, axis_at), (shards_of,), jnp.float32, low / len(cuts), top_value / len(cuts)))
        level = level * jnp.repeat(heights, extent[axis_at] // shards_of).reshape([-1 if axis == axis_at else 1 for axis in range(len(extent))])
    return level


def bell_draw(own_key, shape, deviation, limit, pieces=(), held_as=jnp.bfloat16):
    values = jax.random.normal(own_key, shape, jnp.float32) * deviation
    if len(pieces) > 0:
        values = block_levels(own_key, shape, pieces, -0.22, 0.18) * values
    return jnp.clip(values, min=-limit, max=limit).astype(held_as)


def setup_inputs(seed: int = 0) -> dict:
    key_of = jax.random.split(jax.random.key(seed), 16)
    tokens = draw_tokens(jax.random.fold_in(key_of[15], 71), 0)
    norm_gain = jnp.clip(1.0 + 0.18 * jax.random.normal(key_of[1], (D,), jnp.float32), 0.1, 1.9)
    w_gate = bell_draw(key_of[2], (D, HW), D ** -0.5, 0.125, ((0, 8), (1, 4)))
    w_value = bell_draw(key_of[3], (D, HW), D ** -0.5, 0.125, ((0, 8), (1, 4)))
    w_write = bell_draw(key_of[4], (D, GROUPS * STATE), D ** -0.5, 0.125, ((0, 8), (1, 4)))
    w_read = bell_draw(key_of[5], (D, GROUPS * STATE), D ** -0.5, 0.125, ((0, 8), (1, 4)))
    w_step = bell_draw(key_of[6], (D, HEADS), D ** -0.5, 0.125)
    conv_value = bell_draw(key_of[7], (CONV, HW), CONV ** -0.5, 3.0, (), jnp.float32)
    conv_write = bell_draw(key_of[8], (CONV, GROUPS * STATE), CONV ** -0.5, 3.0, (), jnp.float32)
    conv_read = bell_draw(key_of[9], (CONV, GROUPS * STATE), CONV ** -0.5, 3.0, (), jnp.float32)
    step_bias = draw_step_bias(jax.random.fold_in(key_of[15], 71), 0)
    decay_log = jnp.clip(jax.random.uniform(key_of[11], (HEADS,), jnp.float32, 0.0, 0.7), 0.0, 0.7)
    skip_gain = jnp.clip(1.0 + 0.18 * jax.random.normal(key_of[12], (HEADS,), jnp.float32), 0.1, 1.9)
    out_gain = jnp.clip(1.0 + 0.18 * jax.random.normal(key_of[13], (HW,), jnp.float32), 0.1, 1.9)
    w_out = bell_draw(key_of[14], (HW, D), HW ** -0.5, 0.09375, ((1, 8),))
    return {"tokens": tokens, "norm_gain": norm_gain, "w_gate": w_gate, "w_value": w_value, "w_write": w_write, "w_read": w_read, "w_step": w_step, "conv_value": conv_value, "conv_write": conv_write, "conv_read": conv_read, "step_bias": step_bias, "decay_log": decay_log, "skip_gain": skip_gain, "out_gain": out_gain, "w_out": w_out}


EPSILON = 1e-06
HIGHEST = lax.Precision.HIGHEST

def rms_scale(values, gain_vec):
    return values * lax.rsqrt(lax.optimization_barrier(jnp.mean(values * values, axis=-1, keepdims=True)) + EPSILON) * gain_vec

def causal_conv(values, kernel):
    tap_count = kernel.shape[0]
    length = values.shape[1]
    padded = jnp.pad(values, ((0, 0), (tap_count - 1, 0), (0, 0)))
    running = jnp.zeros_like(values)
    for offset in range(tap_count):
        running = running + padded[:, offset:offset + length, :] * kernel[offset]
    return jax.nn.silu(running)

def blockwise_state(value_conv, step_size, decay_rate, write_conv, read_conv):
    seq_count, length = (step_size.shape[0], step_size.shape[1])
    block_count = length // BLOCK
    repeat_heads = HEADS // GROUPS

    def split_blocks(values, tail_shape):
        return jnp.moveaxis(values.reshape((seq_count, block_count, BLOCK) + tail_shape), 1, 0)
    value_blocks = split_blocks(value_conv, (HEADS, HEAD_DIM))
    step_blocks = split_blocks(step_size, (HEADS,))
    write_blocks = split_blocks(write_conv, (GROUPS, STATE))
    read_blocks = split_blocks(read_conv, (GROUPS, STATE))
    causal_mask = jnp.arange(BLOCK)[:, None] >= jnp.arange(BLOCK)[None, :]

    def one_block(state, inputs):
        value_b, step_b, write_b, read_b = inputs
        write_heads = jnp.repeat(write_b, repeat_heads, axis=2)
        read_heads = jnp.repeat(read_b, repeat_heads, axis=2)
        log_decay = jnp.cumsum(step_b * decay_rate, axis=1)
        value_steps = value_b * step_b[..., None]
        log_gap = log_decay[:, :, None, :] - log_decay[:, None, :, :]
        weights = jnp.exp(jnp.where(causal_mask[None, :, :, None], log_gap, -jnp.inf))
        scores = jnp.einsum('slhn,smhn->slmh', read_heads, write_heads, precision=HIGHEST) * weights
        inner = jnp.einsum('slmh,smhp->slhp', scores, value_steps, precision=HIGHEST)
        carried = jnp.einsum('slhn,shpn->slhp', read_heads, state, precision=HIGHEST) * jnp.exp(log_decay)[..., None]
        block_decay = log_decay[:, -1, :]
        fade_out = jnp.exp(block_decay[:, None, :] - log_decay)
        state = state * jnp.exp(block_decay)[..., None, None] + jnp.einsum('smhn,smh,smhp->shpn', write_heads, fade_out, value_steps, precision=HIGHEST)
        return (state, inner + carried)
    initial = jnp.zeros((seq_count, HEADS, HEAD_DIM, STATE), jnp.float32)
    final_state, outputs = lax.scan(one_block, initial, (value_blocks, step_blocks, write_blocks, read_blocks))
    return jnp.moveaxis(outputs, 0, 1).reshape(seq_count, length, HEADS, HEAD_DIM)

def reference(tokens, norm_gain, w_gate, w_value, w_write, w_read, w_step, conv_value, conv_write, conv_read, step_bias, decay_log, skip_gain, out_gain, w_out):
    seq_count, length, model_width = tokens.shape
    flat_tokens = tokens.astype(jnp.float32).reshape(seq_count * length, model_width)
    normed = rms_scale(flat_tokens, norm_gain).astype(jnp.bfloat16)

    def project(weight):
        result = jnp.dot(normed, weight, preferred_element_type=jnp.float32).astype(jnp.bfloat16)
        result = lax.optimization_barrier(result)
        return result.reshape(seq_count, length, weight.shape[1])
    gate_in = project(w_gate)
    value_in = project(w_value)
    write_in = project(w_write)
    read_in = project(w_read)
    step_raw = jnp.dot(normed, w_step, preferred_element_type=jnp.float32).reshape(seq_count, length, HEADS)
    value_conv = causal_conv(value_in.astype(jnp.float32), conv_value)
    write_conv = causal_conv(write_in.astype(jnp.float32), conv_write)
    read_conv = causal_conv(read_in.astype(jnp.float32), conv_read)
    step_size = jax.nn.softplus(step_raw + step_bias)
    decay_rate = -jnp.exp(decay_log)
    heads_out = blockwise_state(value_conv, step_size, decay_rate, write_conv, read_conv)
    value_heads = value_conv.reshape(seq_count, length, HEADS, HEAD_DIM)
    heads_out = heads_out + skip_gain[:, None] * value_heads
    gated = (heads_out.reshape(seq_count, length, HW) * jax.nn.silu(gate_in.astype(jnp.float32))).astype(jnp.bfloat16)
    gated = lax.optimization_barrier(gated)
    mixed_in = rms_scale(gated.astype(jnp.float32), out_gain).astype(jnp.bfloat16)
    result = jnp.dot(mixed_in.reshape(seq_count * length, HW), w_out, preferred_element_type=jnp.float32)
    return result.astype(jnp.bfloat16).reshape(seq_count, length, model_width)
```

```python
import jax
import jax.numpy as jnp
from jax import lax
from jax.experimental import pallas as pl
from jax.experimental.pallas import tpu as pltpu
from jax.sharding import PartitionSpec as P

EPSILON = 1e-06
HIGHEST = lax.Precision.HIGHEST
HALO = 16
LANES = 128


def shifted(x, axis, by):
    devices = lax.axis_size(axis)
    pairs = [(i, i + by) for i in range(devices) if i + by < devices]
    return lax.ppermute(x, axis, pairs)


def swapped(x, axis, bit):
    devices = lax.axis_size(axis)
    return lax.ppermute(x, axis, [(i, i ^ bit) for i in range(devices)])


def bits_of(axis):
    devices = lax.axis_size(axis)
    bits = []
    bit = devices // 2
    while bit >= 1:
        bits.append(bit)
        bit //= 2
    return bits


def is_power(n):
    return n & (n - 1) == 0


def gather_tokens(x, axis):
    seqs, rows, width = x.shape
    devices = lax.axis_size(axis)
    if not is_power(devices):
        return lax.all_gather(x, axis, axis=1, tiled=True)
    rank = lax.axis_index(axis)
    held = x.reshape(seqs, 1, rows, width)
    for bit in bits_of(axis):
        other = swapped(held, axis, bit)
        upper = (rank & bit) != 0
        first = jnp.where(upper, other, held)
        second = jnp.where(upper, held, other)
        count = held.shape[1]
        held = jnp.stack([first, second], axis=2).reshape(seqs, 2 * count, rows, width)
    return held.reshape(seqs, devices * rows, width)


def total_over(x, axis):
    devices = lax.axis_size(axis)
    if not is_power(devices):
        return jnp.sum(lax.all_gather(x, axis), axis=0)
    for bit in bits_of(axis):
        x = x + swapped(x, axis, bit)
    return x


def incoming_state(state, decay, axis):
    devices = lax.axis_size(axis)
    whole, whole_decay = state, decay
    before, before_decay = None, None
    step = 1
    while step < devices:
        got = shifted(whole.astype(jnp.bfloat16), axis, step).astype(jnp.float32)
        got_decay = shifted(whole_decay, axis, step)
        if before is None:
            before, before_decay = got, got_decay
        else:
            before = got * before_decay + before
            before_decay = got_decay * before_decay
        whole = got * whole_decay + whole
        whole_decay = got_decay * whole_decay
        step *= 2
    if before is None:
        return jnp.zeros_like(state)
    return before


def silu(v):
    return v / (1.0 + jnp.exp(-v))


def dot32(a, b):
    return jnp.dot(a, b, preferred_element_type=jnp.float32)


def mixer_kernel(head_dim, taps_ref, skip_ref, ext_ref, ld_ref, ldt_ref, step_ref, heads_ref, read_ref, state_ref):
    rows = heads_ref.shape[1]
    channels = heads_ref.shape[2]
    state_dim = read_ref.shape[2]
    tap_count = taps_ref.shape[0]
    per = LANES // head_dim
    at = pl.program_id(1)
    start = pl.multiple_of(at * rows, rows)

    @pl.when(at == 0)
    def _():
        state_ref[...] = jnp.zeros_like(state_ref)

    def conv(first, width):
        ext = ext_ref[0, pl.ds(start, rows + HALO), first : first + width].astype(jnp.float32)
        base = HALO - tap_count + 1
        running = None
        for k in range(tap_count):
            term = ext[base + k : base + k + rows] * taps_ref[k : k + 1, first : first + width]
            running = term if running is None else running + term
        return silu(running)

    write = conv(channels, state_dim)
    read = conv(channels + state_dim, state_dim).astype(jnp.bfloat16)
    read_ref[0] = read
    write_t = write.T.astype(jnp.bfloat16)
    cross = dot32(read, write_t)
    line = lax.broadcasted_iota(jnp.int32, (rows, rows), 0)
    column = lax.broadcasted_iota(jnp.int32, (rows, rows), 1)
    causal = line >= column
    log_decay = ld_ref[0]
    log_decay_t = ldt_ref[0]
    steps = step_ref[0]
    lane = lax.broadcasted_iota(jnp.int32, (rows, LANES), 1) // head_dim

    def spread(values, first):
        out = jnp.broadcast_to(values[:, first : first + 1], (values.shape[0], LANES))
        for i in range(1, per):
            part = jnp.broadcast_to(values[:, first + i : first + i + 1], (values.shape[0], LANES))
            out = jnp.where(lane[: values.shape[0]] == i, part, out)
        return out

    for j in range(channels // LANES):
        cols = slice(j * LANES, (j + 1) * LANES)
        value = conv(j * LANES, LANES)
        scaled = value * spread(steps, j * per)
        scaled_b = scaled.astype(jnp.bfloat16)
        inner = None
        for i in range(per):
            h = j * per + i
            gap = log_decay[:, h : h + 1] - log_decay_t[h : h + 1, :]
            score = cross * jnp.exp(jnp.where(causal, gap, -jnp.inf))
            part = dot32(score.astype(jnp.bfloat16), scaled_b)
            inner = part if inner is None else jnp.where(lane == i, part, inner)
        ld = spread(log_decay, j * per)
        last = ld[rows - 1 : rows, :]
        state = state_ref[0, :, cols]
        carried = dot32(read, state.astype(jnp.bfloat16)) * jnp.exp(ld)
        heads_ref[0, :, cols] = inner + carried + skip_ref[:, cols] * value
        faded = (scaled * jnp.exp(last - ld)).astype(jnp.bfloat16)
        state_ref[0, :, cols] = state * jnp.exp(last) + dot32(write_t, faded)


def gate_kernel(head_dim, heads_ref, read_ref, incoming_ref, reach_ref, gate_ref, gated_ref, square_ref):
    rows, channels = heads_ref.shape[1], heads_ref.shape[2]
    per = LANES // head_dim
    read = read_ref[0]
    reach = jnp.exp(reach_ref[0])
    lane = lax.broadcasted_iota(jnp.int32, (rows, LANES), 1) // head_dim
    squares = jnp.zeros((rows, LANES), jnp.float32)
    for j in range(channels // LANES):
        cols = slice(j * LANES, (j + 1) * LANES)
        scale = jnp.broadcast_to(reach[:, j * per : j * per + 1], (rows, LANES))
        for i in range(1, per):
            h = j * per + i
            scale = jnp.where(lane == i, jnp.broadcast_to(reach[:, h : h + 1], (rows, LANES)), scale)
        outer = dot32(read, incoming_ref[0, :, cols]) * scale
        gate = gate_ref[0, :, cols].astype(jnp.float32)
        gated = ((heads_ref[0, :, cols] + outer) * silu(gate)).astype(jnp.bfloat16)
        gated_ref[0, :, cols] = gated
        wide = gated.astype(jnp.float32)
        squares = squares + wide * wide
    square_ref[0] = jnp.broadcast_to(jnp.sum(squares, axis=1, keepdims=True), (rows, LANES))


def block_spec(rows, width):
    return pl.BlockSpec((1, rows, width), lambda s, b: (s, b, 0))


def seq_spec(rows, width):
    return pl.BlockSpec((1, rows, width), lambda s, b: (s, 0, 0))


def body(
    tokens,
    norm_gain,
    w_gate,
    w_value,
    w_write,
    w_read,
    w_step,
    conv_value,
    conv_write,
    conv_read,
    step_bias,
    decay_log,
    skip_gain,
    out_gain,
    w_out,
):
    seqs, own_rows, width = tokens.shape
    group = lax.axis_size("tp")
    rank = lax.axis_index("tp")
    local_heads = w_step.shape[1] // group
    channels = w_gate.shape[1]
    head_dim = channels // local_heads
    state_dim = w_write.shape[1]
    tap_count = conv_value.shape[0]
    rows = own_rows * group
    first_head = rank * local_heads

    def local(x, count, axis):
        return lax.dynamic_slice_in_dim(x, rank * count, count, axis)

    mix_part = jnp.concatenate([w_value, w_write, w_read], axis=1)
    w_mix = lax.all_gather(mix_part, "sp", axis=0, tiled=True)
    gate_part, w_mix = lax.optimization_barrier((w_gate, w_mix))
    whole_gate = lax.all_gather(gate_part, "sp", axis=0, tiled=True)
    out_part, whole_gate = lax.optimization_barrier((local(w_out, channels, 0), whole_gate))
    whole_out = lax.all_gather(out_part, "sp", axis=1, tiled=True)

    wide = tokens.astype(jnp.float32)
    scale = lax.rsqrt(jnp.mean(wide * wide, axis=-1, keepdims=True) + EPSILON)
    normed = (wide * scale * norm_gain).astype(jnp.bfloat16)
    flat = gather_tokens(normed, "tp").reshape(seqs * rows, width)

    step_raw = dot32(flat, local(w_step, local_heads, 1)).reshape(seqs, rows, local_heads)
    step_size = jax.nn.softplus(step_raw + local(step_bias, local_heads, 0))
    rate = -jnp.exp(local(decay_log, local_heads, 0))
    block = LANES if rows % LANES == 0 else rows
    blocks = rows // block
    lower = jnp.tril(jnp.ones((block, block), jnp.float32))
    change = (step_size * rate).reshape(seqs, blocks, block, local_heads)
    log_decay = jnp.einsum("lm,skmh->sklh", lower, change, precision=HIGHEST)
    log_decay_t = jnp.moveaxis(log_decay, 3, 1).reshape(seqs, local_heads, rows)
    block_total = log_decay[:, :, -1, :]
    run_sum = jnp.cumsum(block_total, axis=1)
    reach = ((run_sum - block_total)[:, :, None, :] + log_decay).reshape(seqs, rows, local_heads)
    log_decay = log_decay.reshape(seqs, rows, local_heads)
    dev_decay = jnp.repeat(jnp.exp(run_sum[:, -1:, :]), head_dim, axis=2)

    taps = jnp.concatenate(
        [local(conv_value, channels, 1), local(conv_write, state_dim, 1), local(conv_read, state_dim, 1)], axis=1
    )
    skip = jnp.repeat(local(skip_gain, local_heads, 0), head_dim)[None]

    mix = dot32(flat, w_mix).astype(jnp.bfloat16).reshape(seqs, rows, w_mix.shape[1])
    tail = shifted(mix[:, rows - tap_count + 1 :], "sp", 1)
    ext = jnp.concatenate([jnp.pad(tail, ((0, 0), (HALO - tap_count + 1, 0), (0, 0))), mix], axis=1)

    grid = (seqs, blocks)
    full = lambda a: pl.BlockSpec(a.shape, lambda s, b: (0,) * a.ndim)
    params = pltpu.CompilerParams(dimension_semantics=("arbitrary", "arbitrary"))
    heads, read_rows, state = pl.pallas_call(
        lambda *refs: mixer_kernel(head_dim, *refs),
        grid=grid,
        in_specs=[
            full(taps),
            full(skip),
            seq_spec(rows + HALO, ext.shape[2]),
            block_spec(block, local_heads),
            pl.BlockSpec((1, local_heads, block), lambda s, b: (s, 0, b)),
            block_spec(block, local_heads),
        ],
        out_specs=[block_spec(block, channels), block_spec(block, state_dim), seq_spec(state_dim, channels)],
        out_shape=[
            jax.ShapeDtypeStruct((seqs, rows, channels), jnp.float32),
            jax.ShapeDtypeStruct((seqs, rows, state_dim), jnp.bfloat16),
            jax.ShapeDtypeStruct((seqs, state_dim, channels), jnp.float32),
        ],
        compiler_params=params,
        cost_estimate=pl.CostEstimate(flops=20 * 10**9, bytes_accessed=8 * 2**20, transcendentals=0),
        name="mixer",
    )(taps, skip, ext, log_decay, log_decay_t, step_size)

    incoming = incoming_state(state, dev_decay, "sp").astype(jnp.bfloat16)

    gate_in = dot32(flat, whole_gate).astype(jnp.bfloat16).reshape(seqs, rows, channels)
    gated, squares = pl.pallas_call(
        lambda *refs: gate_kernel(head_dim, *refs),
        grid=grid,
        in_specs=[
            block_spec(block, channels),
            block_spec(block, state_dim),
            seq_spec(state_dim, channels),
            block_spec(block, local_heads),
            block_spec(block, channels),
        ],
        out_specs=[block_spec(block, channels), block_spec(block, LANES)],
        out_shape=[
            jax.ShapeDtypeStruct((seqs, rows, channels), jnp.bfloat16),
            jax.ShapeDtypeStruct((seqs, rows, LANES), jnp.float32),
        ],
        compiler_params=params,
        cost_estimate=pl.CostEstimate(flops=5 * 10**9, bytes_accessed=8 * 2**20, transcendentals=0),
        name="gating",
    )(heads, read_rows, incoming, reach, gate_in)

    square_sum = total_over(squares[:, :, :1], "tp")
    out_scale = lax.rsqrt(square_sum / (channels * group) + EPSILON)
    mixed_in = (gated.astype(jnp.float32) * out_scale * local(out_gain, channels, 0)).astype(jnp.bfloat16)

    if not is_power(group):
        partial = dot32(mixed_in.reshape(seqs * rows, channels), whole_out).reshape(seqs, rows, width)
        return lax.psum_scatter(partial, "tp", scatter_dimension=1, tiled=True).astype(jnp.bfloat16)

    bits = bits_of("tp")[::-1]
    pieces = mixed_in.reshape(seqs, group // 2, 2, own_rows, channels)

    def product(which):
        chosen = lax.dynamic_index_in_dim(pieces, which, 2, False)
        return dot32(chosen.reshape(-1, channels), whole_out).reshape(seqs, group // 2, own_rows, width)

    mine = rank & 1
    send = product(1 - mine).astype(jnp.bfloat16)
    got = swapped(send, "tp", 1)
    keep = product(mine) + got.astype(jnp.float32)
    for bit in bits[1:]:
        count = keep.shape[1]
        split = keep.reshape(seqs, count // 2, 2, own_rows, width)
        side = (rank // bit) & 1
        send = lax.dynamic_index_in_dim(split, 1 - side, 2, False).astype(jnp.bfloat16)
        kept = lax.dynamic_index_in_dim(split, side, 2, False)
        keep = kept + swapped(send, "tp", bit).astype(jnp.float32)
    return keep.reshape(seqs, own_rows, width).astype(jnp.bfloat16)


def solution(mesh):
    in_specs = (
        P(None, ("sp", "tp"), None),
        P(),
        P("sp", "tp"),
        P("sp", "tp"),
        P("sp", "tp"),
        P("sp", "tp"),
        P(),
        P(),
        P(),
        P(),
        P(),
        P(),
        P(),
        P(),
        P(None, "sp"),
    )
    out_specs = P(None, ("sp", "tp"), None)
    return jax.shard_map(body, mesh=mesh, in_specs=in_specs, out_specs=out_specs, check_vma=False)
```
